32 devices in a mesh: sp: 8 (over z, x), tp: 4 (over y, core).
Axes of the slice: x: 2, y: 2, z: 4, core: 2. Of those that a mesh axis runs over, the one named last changes fastest.
Arguments:
- tokens: bfloat16 [8192, 2048], P('sp'), may hold values from -6 to 6
- pre_gain: float32 [2048], replicated, may hold values from 0.1 to 1.9
- w_query: bfloat16 [2048, 2048], P(None, 'tp'), may hold values from -0.125 to 0.125
- w_key: bfloat16 [2048, 2048], P(None, 'tp'), may hold values from -0.125 to 0.125
- w_value: bfloat16 [2048, 2048], P(None, 'tp'), may hold values from -0.125 to 0.125
- memory_output_gate_weight: bfloat16 [2048, 2048], P(None, 'tp'), may hold values from -0.125 to 0.125
- w_input_gate: bfloat16 [2048, 8], replicated, may hold values from -0.125 to 0.125
- w_forget_gate: bfloat16 [2048, 8], replicated, may hold values from -0.125 to 0.125
- input_bias: float32 [8], replicated, may hold values from -3 to 220
- forget_bias: float32 [8], replicated, may hold values from 3.9 to 12.4
- forget_extra: float32 [8192, 8], P('sp', 'tp'), may hold values from -1.5 to 0
- initial_memory: float32 [8, 256, 256], P('tp', 'sp'), may hold values from -2048 to 2048
- initial_normal: float32 [8, 256], P('tp', 'sp'), may hold values from -2048 to 2048
- memory_gain: float32 [2048], replicated, may hold values from 0.1 to 1.9
- w_pool_input: bfloat16 [2048, 1024], P(None, 'tp'), may hold values from -0.125 to 0.125
- w_pool_gate: bfloat16 [2048, 1024], P(None, 'tp'), may hold values from -0.125 to 0.125
- pool_mix: bfloat16 [8, 128, 128], replicated, may hold values from -0.5 to 0.5
- pool_gain: float32 [1024], replicated, may hold values from 0.1 to 1.9
- w_out_memory: bfloat16 [2048, 2048], P('tp'), may hold values from -0.109375 to 0.109375
- w_out_pool: bfloat16 [1024, 2048], P('tp'), may hold values from -0.109375 to 0.109375
- post_gain: float32 [2048], replicated, may hold values from 0.1 to 1.9
Outputs:
- layer_out: bfloat16 [8192, 2048], P(('sp', 'tp'))
The draws below stay inside these ranges and needn't reach their ends.
All inputs are finite; a program needn't handle non-finite values.
Results may differ from the reference program's by a relative error of at most 0.018.
The reference program's roundings to bfloat16 on the way count: a program that leaves them out, or rounds other values in their place, can miss the bound.
Values may be sent and summed in bfloat16 or wider, within the bound.
A program may use at most 128 MiB of HBM per device.

```python
import jax
import jax.numpy as jnp
from jax import lax

D = 2048
HEADS = 8
HEAD_DIM = 256
MEM_WIDTH = 2048
POOL_GROUPS = 8
GROUP_DIM = 128
POOL_WIDTH = 1024
TOKENS_PER_SHARD = 1024
BLOCK = 512
TOKENS = 8192
N_TP = 4


def draw_input_bias(key, part):
    result = jnp.clip(jax.random.normal(jax.random.fold_in(key, 13), (HEADS,), jnp.float32), -3.0, 3.0)
    return result


def draw_forget_bias(key, part):
    order = jax.random.permutation(jax.random.fold_in(key, 21), HEADS)
    fast_count = HEADS // 2
    slow_value = jnp.log(jnp.float32(TOKENS)) + 1.5 + jax.random.uniform(jax.random.fold_in(key, 22), (HEADS,), jnp.float32, -0.5, 0.5)
    slow_value = jnp.minimum(slow_value, 12.4)
    fast_value = jax.random.uniform(jax.random.fold_in(key, 23), (HEADS,), jnp.float32, 3.9, 4.6)
    return jnp.where(order < fast_count, fast_value, slow_value)


def draw_forget_extra(key, part):
    block_total = TOKENS // TOKENS_PER_SHARD
    rates = jnp.exp(jax.random.uniform(jax.random.fold_in(key, 31), (block_total, HEADS), jnp.float32, jnp.log(0.3), jnp.log(1.2)))
    rough = jax.random.uniform(jax.random.fold_in(key, 32), (TOKENS, HEADS), jnp.float32, 0.5, 1.5)
    baseline = -(jnp.repeat(rates, TOKENS_PER_SHARD, axis=0) * rough) / TOKENS
    spots = jax.random.randint(jax.random.fold_in(key, 33), (2,), 0, TOKENS)
    losses = jax.random.uniform(jax.random.fold_in(key, 34), (2, HEADS), jnp.float32, 0.22, 0.69)
    struck = (jnp.arange(TOKENS)[:, None] == spots[None, :]).astype(jnp.float32)
    return baseline - jnp.dot(struck, losses)


def block_scale(key, shape, pieces, least, top_value):
    def one(dim, parts):
        heights = jax.random.uniform(jax.random.fold_in(jax.random.fold_in(key, 6), dim), (parts,), jnp.float32, least / len(pieces), top_value / len(pieces))
        return jnp.repeat(jnp.exp(heights), shape[dim] // parts).reshape((-1,) + (1,) * (len(shape) - dim - 1))

    factor_of = one(*pieces[0])
    for cut in pieces[1:]:
        factor_of = factor_of * one(*cut)
    return factor_of


def scatter_about(own_key, shape, deviation, limit, shards=(), dtype=jnp.bfloat16):
    values = deviation * jax.random.normal(own_key, shape, jnp.float32)
    if shards:
        values = values * block_scale(own_key, shape, shards, -0.22, 0.18)
    return jnp.clip(values, -limit, limit).astype(dtype)


def setup_inputs(seed: int = 0) -> dict:
    streams_of = jax.random.split(jax.random.key(seed), 22)
    tokens = scatter_about(streams_of[0], (TOKENS, D), 1.0, 6.0, ((0, 8),))
    pre_gain = jnp.clip(1.0 + 0.18 * jax.random.normal(streams_of[1], (D,), jnp.float32), 0.1, 1.9)
    w_query = scatter_about(streams_of[2], (D, MEM_WIDTH), D ** -0.5, 0.125, ((1, 4),))
    w_key = scatter_about(streams_of[3], (D, MEM_WIDTH), D ** -0.5, 0.125, ((1, 4),))
    w_value = scatter_about(streams_of[4], (D, MEM_WIDTH), D ** -0.5, 0.125, ((1, 4),))
    memory_output_gate_weight = scatter_about(streams_of[5], (D, MEM_WIDTH), D ** -0.5, 0.125, ((1, 4),))
    w_input_gate = scatter_about(streams_of[6], (D, HEADS), D ** -0.5, 0.125)
    w_forget_gate = scatter_about(streams_of[7], (D, HEADS), D ** -0.5, 0.125)
    input_bias = draw_input_bias(jax.random.fold_in(streams_of[21], 71), 0)
    forget_bias = draw_forget_bias(jax.random.fold_in(streams_of[21], 71), 0)
    forget_extra = draw_forget_extra(jax.random.fold_in(streams_of[21], 71), 0)
    initial_memory = scatter_about(streams_of[11], (HEADS, HEAD_DIM, HEAD_DIM), (4 * TOKENS ** 0.5), 2048.0, ((0, 4), (1, 8)), jnp.float32)
    initial_normal = scatter_about(streams_of[12], (HEADS, HEAD_DIM), (4 * TOKENS ** 0.5), 2048.0, ((0, 4), (1, 8)), jnp.float32)
    memory_gain = jnp.clip(1.0 + 0.18 * jax.random.normal(streams_of[13], (MEM_WIDTH,), jnp.float32), 0.1, 1.9)
    w_pool_input = scatter_about(streams_of[14], (D, POOL_WIDTH), D ** -0.5, 0.125, ((1, 4),))
    w_pool_gate = scatter_about(streams_of[15], (D, POOL_WIDTH), D ** -0.5, 0.125, ((1, 4),))
    pool_mix = scatter_about(streams_of[16], (POOL_GROUPS, GROUP_DIM, GROUP_DIM), GROUP_DIM ** -0.5, 0.5)
    pool_gain = jnp.clip(1.0 + 0.18 * jax.random.normal(streams_of[17], (POOL_WIDTH,), jnp.float32), 0.1, 1.9)
    w_out_memory = scatter_about(streams_of[18], (MEM_WIDTH, D), (MEM_WIDTH + POOL_WIDTH) ** -0.5, 0.109375, ((0, 4),))
    w_out_pool = scatter_about(streams_of[19], (POOL_WIDTH, D), (MEM_WIDTH + POOL_WIDTH) ** -0.5, 0.109375, ((0, 4),))
    post_gain = jnp.clip(1.0 + 0.18 * jax.random.normal(streams_of[20], (D,), jnp.float32), 0.1, 1.9)
    return dict(tokens=tokens, pre_gain=pre_gain, w_query=w_query, w_key=w_key, w_value=w_value, memory_output_gate_weight=memory_output_gate_weight, w_input_gate=w_input_gate, w_forget_gate=w_forget_gate, input_bias=input_bias, forget_bias=forget_bias, forget_extra=forget_extra, initial_memory=initial_memory, initial_normal=initial_normal, memory_gain=memory_gain, w_pool_input=w_pool_input, w_pool_gate=w_pool_gate, pool_mix=pool_mix, pool_gain=pool_gain, w_out_memory=w_out_memory, w_out_pool=w_out_pool, post_gain=post_gain)


EPS = 1e-06

def normalize(values, gain):
    return values * lax.rsqrt(lax.optimization_barrier(jnp.mean(values * values, axis=-1, keepdims=True)) + EPS) * gain

def block_parts(memory_carry, block_inputs):
    matrix_memory_state, memory_normal, stabilizer = memory_carry
    queries, keys_in, incoming_values, log_input, log_keep = block_inputs
    length = queries.shape[1]
    head_scale = queries.shape[2] ** (-0.5)
    causal = jnp.arange(length)[:, None] >= jnp.arange(length)[None, :]
    running_keep = jnp.cumsum(log_keep, axis=-1)
    decayed = jnp.where(causal[None], running_keep[:, :, None] - running_keep[:, None, :] + log_input[:, None, :], -jnp.inf)
    carried = running_keep + stabilizer[:, None]
    row_max = jnp.maximum(lax.optimization_barrier(jnp.max(decayed, axis=-1)), carried)
    wide_queries = queries.astype(jnp.float32)
    broadcast_values = incoming_values.astype(jnp.float32)
    wide_keys = keys_in.astype(jnp.float32)
    scores = jnp.einsum('hld,hsd->hls', wide_queries, wide_keys)
    weights = jnp.exp(decayed - row_max[:, :, None]) * scores * head_scale
    carry_weight = jnp.exp(carried - row_max) * head_scale
    rounded = lax.optimization_barrier(weights.astype(jnp.bfloat16)).astype(jnp.float32)
    numerator = jnp.einsum('hls,hsd->hld', rounded, broadcast_values)
    numerator = numerator + carry_weight[:, :, None] * jnp.einsum('hld,hde->hle', wide_queries, matrix_memory_state, precision=lax.Precision.HIGHEST)
    denominator = lax.optimization_barrier(jnp.sum(weights, axis=-1)) + carry_weight * jnp.einsum('hld,hd->hl', wide_queries, memory_normal, precision=lax.Precision.HIGHEST)
    block_keep = running_keep[:, -1]
    write_log = block_keep[:, None] - running_keep + log_input
    new_stabilizer = jnp.maximum(block_keep + stabilizer, lax.optimization_barrier(jnp.max(write_log, axis=-1)))
    decay_factor = jnp.exp(block_keep + stabilizer - new_stabilizer)
    write_weight = jnp.exp(write_log - new_stabilizer[:, None])
    key_projected = write_weight[:, :, None] * wide_keys
    key_projected_rounded = lax.optimization_barrier(key_projected.astype(jnp.bfloat16)).astype(jnp.float32)
    matrix_memory_state = decay_factor[:, None, None] * matrix_memory_state + jnp.einsum('gbq,gbd->gqd', key_projected_rounded, broadcast_values)
    memory_normal = decay_factor[:, None] * memory_normal + lax.optimization_barrier(jnp.sum(key_projected, axis=1))
    return ((matrix_memory_state, memory_normal, new_stabilizer), (numerator, denominator, row_max))

def reference(tokens, pre_gain, w_query, w_key, w_value, memory_output_gate_weight, w_input_gate, w_forget_gate, input_bias, forget_bias, forget_extra, initial_memory, initial_normal, memory_gain, w_pool_input, w_pool_gate, pool_mix, pool_gain, w_out_memory, w_out_pool, post_gain):
    normed = normalize(tokens.astype(jnp.float32), pre_gain).astype(jnp.bfloat16)

    def by_heads(weight):
        product = jnp.dot(normed, weight, preferred_element_type=jnp.float32)
        return product.reshape(TOKENS, HEADS, HEAD_DIM).transpose(1, 0, 2)
    queries = by_heads(w_query).astype(jnp.bfloat16)
    keys_all = by_heads(w_key).astype(jnp.bfloat16)
    values_all = by_heads(w_value).astype(jnp.bfloat16)
    memory_gate = by_heads(memory_output_gate_weight)
    log_input = (jnp.dot(normed, w_input_gate, preferred_element_type=jnp.float32) + input_bias).T
    log_keep = (jax.nn.log_sigmoid(jnp.dot(normed, w_forget_gate, preferred_element_type=jnp.float32) + forget_bias) + forget_extra).T
    block_total = TOKENS // BLOCK

    def split(array):
        return jnp.moveaxis(array.reshape((HEADS, block_total, BLOCK) + array.shape[2:]), 1, 0)

    def join(array):
        return jnp.moveaxis(array, 0, 1).reshape((HEADS, TOKENS) + array.shape[3:])
    begin = (initial_memory, initial_normal, jnp.zeros((HEADS,), jnp.float32))
    _, (numerator, denominator, row_max) = lax.scan(block_parts, begin, (split(queries), split(keys_all), split(values_all), split(log_input), split(log_keep)))
    numerator, denominator, row_max = (join(numerator), join(denominator), join(row_max))
    memory_rows = numerator / jnp.maximum(jnp.abs(denominator), jnp.exp(-row_max))[..., None]
    row_scale = lax.rsqrt(lax.optimization_barrier(jnp.mean(memory_rows * memory_rows, axis=(0, 2), keepdims=True)) + EPS)
    memory_out = (memory_rows * row_scale * memory_gain.reshape(HEADS, 1, HEAD_DIM) * jax.nn.silu(memory_gate)).astype(jnp.bfloat16)
    memory_out = memory_out.transpose(1, 0, 2).reshape(TOKENS, MEM_WIDTH)
    pool_input = jnp.dot(normed, w_pool_input, preferred_element_type=jnp.float32).astype(jnp.bfloat16)
    grouped = pool_input.astype(jnp.float32).reshape(TOKENS, POOL_GROUPS, GROUP_DIM)
    running = jnp.concatenate([jnp.zeros((1, POOL_GROUPS, GROUP_DIM), jnp.float32), jnp.cumsum(grouped, axis=0)], axis=0)
    position = (jnp.arange(TOKENS) + 1).astype(jnp.int32)[:, None]
    windows = (2 ** (jnp.arange(POOL_GROUPS) + 1)).astype(jnp.int32)[None, :]
    lowest = jnp.maximum(position - windows, 0).astype(jnp.int32)
    group_ids = jnp.arange(POOL_GROUPS).astype(jnp.int32)[None, :]
    window_sums = running[1:] - running[lowest, group_ids]
    counts = (position - lowest).astype(jnp.float32)
    pooled = (window_sums / counts[..., None] - grouped).astype(jnp.bfloat16)
    mixed = jnp.einsum('tgc,gce->tge', pooled.astype(jnp.float32), pool_mix.astype(jnp.float32))
    pool_gate = jnp.dot(normed, w_pool_gate, preferred_element_type=jnp.float32)
    pool_out = (mixed.reshape(TOKENS, POOL_WIDTH) * pool_gain * jax.nn.silu(pool_gate)).astype(jnp.bfloat16)
    memory_cols = MEM_WIDTH // N_TP
    pool_cols = POOL_WIDTH // N_TP
    summed = jnp.zeros((TOKENS, D), jnp.float32)
    for member in range(N_TP):
        low_mem = member * memory_cols
        low_pool = member * pool_cols
        partial_value = jnp.dot(memory_out[:, low_mem:low_mem + memory_cols], w_out_memory[low_mem:low_mem + memory_cols], preferred_element_type=jnp.float32)
        partial_value = partial_value + jnp.dot(pool_out[:, low_pool:low_pool + pool_cols], w_out_pool[low_pool:low_pool + pool_cols], preferred_element_type=jnp.float32)
        summed = summed + lax.optimization_barrier(partial_value.astype(jnp.bfloat16)).astype(jnp.float32)
    return normalize(summed, post_gain).astype(jnp.bfloat16)
```

```python
import functools

import jax
import jax.numpy as jnp
from jax import lax
from jax.experimental import pallas as pl
from jax.experimental.pallas import tpu as pltpu
from jax.sharding import PartitionSpec as P

HEAD_DIM = 256
GROUP_DIM = 128
WIDEST = 256
TILE = 256
CHUNKS = 2
EPS = 1e-06
FLOOR = -1e30
F32 = jnp.float32
BF16 = jnp.bfloat16
MESH = pl.DeviceIdType.MESH


def dot(a, b):
    return jnp.dot(a, b, preferred_element_type=F32)


def silu(x):
    return x / (1.0 + jnp.exp(-x))


def kernel(
    n_sp,
    n_tp,
    tokens_hbm,
    gain_ref,
    wq_hbm,
    wk_hbm,
    wv_hbm,
    wg_hbm,
    gates_w_ref,
    gates_b_ref,
    extra_ref,
    init_ref,
    normal_ref,
    mem_gain_ref,
    wpi_hbm,
    wpg_hbm,
    mix_ref,
    pool_gain_ref,
    wom_hbm,
    wop_hbm,
    post_ref,
    out_ref,
    tokens,
    wq,
    wk,
    wv,
    wg,
    wpi,
    wpg,
    wom,
    wop,
    normed,
    q_ref,
    k_ref,
    v_ref,
    gate_ref,
    pgate_ref,
    ext_ref,
    pool_ref,
    rows_ref,
    cols_ref,
    num_ref,
    den_ref,
    max_ref,
    s_send,
    s_recv,
    a_send,
    a_recv,
    e_send,
    e_recv,
    sq_send,
    sq_recv,
    scale_ref,
    sib_send,
    sib_recv,
    own_ref,
    link_send,
    link_recv,
    local_sem,
    s_sems,
    a_sems,
    e_sems,
    halo_sems,
    sq_sems,
    sib_sems,
    link_sems,
):
    T, D = tokens.shape
    H = q_ref.shape[0]
    G = pool_ref.shape[1] // GROUP_DIM
    sp = lax.axis_index("sp")
    tp = lax.axis_index("tp")
    head_scale = HEAD_DIM ** (-0.5)
    tiles = T // TILE

    loads = {}
    for slot, (name, src, dst) in enumerate(
        [
            ("tokens", tokens_hbm, tokens),
            ("wk", wk_hbm, wk),
            ("wv", wv_hbm, wv),
            ("wpi", wpi_hbm, wpi),
            ("wq", wq_hbm, wq),
            ("wg", wg_hbm, wg),
            ("wpg", wpg_hbm, wpg),
            ("wop", wop_hbm, wop),
            ("wom", wom_hbm, wom),
        ]
    ):
        loads[name] = pltpu.make_async_copy(src, dst, local_sem.at[slot])
        loads[name].start()

    barrier = pltpu.get_barrier_semaphore()
    for step in range(1, n_sp):
        pl.semaphore_signal(
            barrier, inc=1, device_id={"sp": lax.rem(sp + step, n_sp)}, device_id_type=MESH
        )
    for step in range(1, n_tp):
        pl.semaphore_signal(
            barrier, inc=1, device_id={"tp": lax.rem(tp + step, n_tp)}, device_id_type=MESH
        )

    def remote(src, dst, sems, slot, axis, peer):
        return pltpu.make_async_remote_copy(
            src_ref=src,
            dst_ref=dst,
            send_sem=sems.at[0, slot],
            recv_sem=sems.at[1, slot],
            device_id={axis: peer},
            device_id_type=MESH,
        )

    def by_tile(body, size=TILE):
        def step(index, carry):
            body(pl.ds(pl.multiple_of(index * size, size), size))
            return carry

        lax.fori_loop(0, T // size, step, 0)

    loads["tokens"].wait()

    def norm_tile(rows):
        x = tokens[rows, :].astype(F32)
        scale = lax.rsqrt(jnp.mean(x * x, axis=-1, keepdims=True) + EPS)
        normed[rows, :] = (x * scale * gain_ref[...]).astype(BF16)

    by_tile(norm_tile, 64)

    def gate_tile(rows):
        cols_ref[rows, :] = dot(normed[rows, :], gates_w_ref[...]) + gates_b_ref[...]

    by_tile(gate_tile)
    tri = (
        lax.broadcasted_iota(jnp.int32, (TILE, TILE), 0)
        <= lax.broadcasted_iota(jnp.int32, (TILE, TILE), 1)
    ).astype(F32)
    rows_ref[...] = jnp.zeros_like(rows_ref)
    carry = jnp.zeros((8, 1), F32)
    for t in range(tiles):
        span = pl.ds(t * TILE, TILE)
        raw = cols_ref[span, :].T[0:8]
        log_keep = jnp.minimum(raw, 0.0) - jnp.log1p(jnp.exp(-jnp.abs(raw))) + extra_ref[:, span]
        run = carry + jnp.dot(
            log_keep, tri, preferred_element_type=F32, precision=lax.Precision.HIGHEST
        )
        carry = run[:, TILE - 1 : TILE]
        rows_ref[0:H, span] = raw[0:H] - run[H : 2 * H]
        rows_ref[H : 2 * H, span] = run[H : 2 * H]
    for t in range(tiles):
        span = pl.ds(t * TILE, TILE)
        cols_ref[span, :] = rows_ref[:, span].T

    def project(name, weight, store):
        loads[name].wait()

        def tile(rows):
            store(rows, dot(normed[rows, :], weight[...]))

        by_tile(tile)

    def heads_to(ref):
        def store(rows, value):
            for h in range(H):
                ref[h, rows, :] = value[:, h * HEAD_DIM : (h + 1) * HEAD_DIM].astype(ref.dtype)

        return store

    project("wk", wk, heads_to(k_ref))
    project("wv", wv, heads_to(v_ref))

    part = HEAD_DIM // n_sp
    a_send[...] = jnp.zeros_like(a_send)
    for h in range(H):
        a_max = jnp.max(rows_ref[h : h + 1, :], axis=-1, keepdims=True)
        total = rows_ref[H + h : H + h + 1, T - 1 : T]
        state = jnp.zeros((HEAD_DIM, HEAD_DIM), F32)
        normal = jnp.zeros((1, HEAD_DIM), F32)
        for t in range(tiles):
            span = pl.ds(t * TILE, TILE)
            weight = jnp.exp(cols_ref[span, h : h + 1] - a_max)
            kw = weight * k_ref[h, span, :].astype(F32)
            normal = normal + jnp.sum(kw, axis=0, keepdims=True)
            state = state + lax.dot_general(
                kw.astype(BF16),
                v_ref[h, span, :],
                (((0,), (0,)), ((), ())),
                preferred_element_type=F32,
            )
        s_send[:, h] = state.reshape(n_sp, part, HEAD_DIM).astype(s_send.dtype)
        a_send[4 * h : 4 * h + 1, :] = jnp.broadcast_to(total + a_max, (1, HEAD_DIM))
        a_send[4 * h + 1 : 4 * h + 2, :] = jnp.broadcast_to(total, (1, HEAD_DIM))
        a_send[4 * h + 2 : 4 * h + 3, :] = normal
        a_send[4 * h + 3 : 4 * h + 4, :] = normal_ref[h : h + 1, :]

    pl.semaphore_wait(barrier, n_sp - 1 + n_tp - 1)
    first = []
    for step in range(1, n_sp):
        peer = lax.rem(sp + step, n_sp)
        first.append(remote(s_send.at[peer], s_recv.at[sp], s_sems, step, "sp", peer))
        first.append(remote(a_send, a_recv.at[sp], a_sems, step, "sp", peer))
    for copy in first:
        copy.start()
    s_recv[sp] = s_send[sp]
    a_recv[sp] = a_send[...]

    def store_pool(rows, value):
        ext_ref[pl.ds(pl.multiple_of(rows.start + WIDEST, TILE), TILE), :] = value.astype(BF16)

    project("wpi", wpi, store_pool)
    halo = remote(
        ext_ref.at[pl.ds(T, WIDEST)],
        ext_ref.at[pl.ds(0, WIDEST)],
        halo_sems,
        0,
        "sp",
        lax.rem(sp + 1, n_sp),
    )
    halo.start()
    project("wq", wq, heads_to(q_ref))
    project("wg", wg, heads_to(gate_ref))

    for copy in first:
        copy.wait()
    enter_max, enter_normal = [], []
    for h in range(H):
        state = init_ref[h].astype(F32)
        normal = jnp.zeros((1, HEAD_DIM), F32)
        for j in range(n_sp):
            normal = normal + a_recv[j, 4 * h + 3 : 4 * h + 4, :]
        stab = jnp.zeros((1, HEAD_DIM), F32)
        my_stab, my_normal = stab, normal
        for j in range(n_sp):
            e_send[j, h] = state.astype(e_send.dtype)
            my_stab = jnp.where(sp == j, stab, my_stab)
            my_normal = jnp.where(sp == j, normal, my_normal)
            late = a_recv[j, 4 * h : 4 * h + 1, :]
            keep = a_recv[j, 4 * h + 1 : 4 * h + 2, :]
            joint = jnp.maximum(late, keep + stab)
            early_factor = jnp.exp(keep + stab - joint)
            late_factor = jnp.exp(late - joint)
            state = state * early_factor + s_recv[j, h].astype(F32) * late_factor
            normal = normal * early_factor + a_recv[j, 4 * h + 2 : 4 * h + 3, :] * late_factor
            stab = joint
        enter_max.append(my_stab[:, 0:1])
        enter_normal.append(my_normal)
    second = []
    for step in range(1, n_sp):
        peer = lax.rem(sp + step, n_sp)
        second.append(remote(e_send.at[peer], e_recv.at[sp], e_sems, step, "sp", peer))
    for copy in second:
        copy.start()
    e_recv[sp] = e_send[sp]

    for h in range(H):
        for t in range(tiles):
            span = pl.ds(t * TILE, TILE)
            width = (t + 1) * TILE
            decayed = cols_ref[span, H + h : H + h + 1] + rows_ref[h : h + 1, 0:width]
            causal = (
                lax.broadcasted_iota(jnp.int32, (TILE, width), 0) + t * TILE
                >= lax.broadcasted_iota(jnp.int32, (TILE, width), 1)
            )
            decayed = jnp.where(causal, decayed, FLOOR)
            row_max = jnp.max(decayed, axis=-1, keepdims=True)
            scores = lax.dot_general(
                q_ref[h, span, :],
                k_ref[h, 0:width, :],
                (((1,), (1,)), ((), ())),
                preferred_element_type=F32,
            )
            weights = jnp.exp(decayed - row_max) * scores * head_scale
            den_ref[h, span, :] = jnp.sum(weights, axis=-1, keepdims=True)
            max_ref[h, span, :] = row_max
            num_ref[h, span, :] = dot(weights.astype(BF16), v_ref[h, 0:width, :])

    def store_gate(rows, value):
        pgate_ref[rows, :] = value

    project("wpg", wpg, store_gate)
    halo.wait()
    for g in range(G):
        window = jnp.left_shift(2, tp * G + g)
        offset = (
            lax.broadcasted_iota(jnp.int32, (TILE, TILE + WIDEST), 0)
            + WIDEST
            - lax.broadcasted_iota(jnp.int32, (TILE, TILE + WIDEST), 1)
        )
        band = jnp.where((offset >= 0) & (offset < window), 1.0, 0.0).astype(BF16)
        lanes = slice(g * GROUP_DIM, (g + 1) * GROUP_DIM)
        for t in range(tiles):
            span = pl.ds(t * TILE, TILE)
            here = ext_ref[t * TILE + WIDEST : (t + 1) * TILE + WIDEST, lanes]
            before = ext_ref[t * TILE : t * TILE + WIDEST, lanes]
            if t == 0:
                before = jnp.where(sp > 0, before.astype(F32), 0.0).astype(BF16)
            sums = dot(band[:, :WIDEST], before) + dot(band[:, WIDEST:], here)
            position = lax.broadcasted_iota(jnp.int32, (TILE, 1), 0) + (sp * T + t * TILE + 1)
            counts = jnp.minimum(position, window).astype(F32)
            pooled = (sums / counts - here.astype(F32)).astype(BF16)
            mixed = dot(pooled, mix_ref[g])
            pool_ref[span, lanes] = (
                mixed * pool_gain_ref[:, lanes] * silu(pgate_ref[span, lanes])
            ).astype(BF16)

    for copy in second:
        copy.wait()
    for t in range(tiles):
        span = pl.ds(t * TILE, TILE)
        squares = jnp.zeros((TILE, 1), F32)
        for h in range(H):
            state = e_recv[:, h].reshape(HEAD_DIM, HEAD_DIM).astype(BF16)
            queries = q_ref[h, span, :]
            carried = cols_ref[span, H + h : H + h + 1] + enter_max[h]
            row_max = max_ref[h, span, :]
            joint = jnp.maximum(row_max, carried)
            local_weight = jnp.exp(row_max - joint)
            carry_weight = jnp.exp(carried - joint) * head_scale
            numerator = num_ref[h, span, :] * local_weight + carry_weight * dot(queries, state)
            denominator = den_ref[h, span, :] * local_weight + carry_weight * jnp.sum(
                queries.astype(F32) * enter_normal[h], axis=-1, keepdims=True
            )
            memory = numerator / jnp.maximum(jnp.abs(denominator), jnp.exp(-joint))
            num_ref[h, span, :] = memory
            squares = squares + jnp.sum(memory * memory, axis=-1, keepdims=True)
        sq_send[:, span] = jnp.broadcast_to(squares, (TILE, 128)).T[0:8]

    third = []
    for step in range(1, n_tp):
        peer = lax.rem(tp + step, n_tp)
        third.append(remote(sq_send, sq_recv.at[step], sq_sems, step, "tp", peer))
    for copy in third:
        copy.start()
    loads["wop"].wait()
    loads["wom"].wait()
    for copy in third:
        copy.wait()
    for t in range(tiles):
        span = pl.ds(t * TILE, TILE)
        total = sq_send[0:1, span]
        for step in range(1, n_tp):
            total = total + sq_recv[step, 0:1, span]
        scale = lax.rsqrt(total / (HEAD_DIM * H * n_tp) + EPS)
        scale_ref[span, :] = jnp.broadcast_to(scale, (128, TILE)).T

    chips = n_tp // 2
    chip, core = tp // 2, lax.rem(tp, 2)
    sibling = chip * 2 + 1 - core
    block = T // n_tp
    size = block // CHUNKS

    def memory_out(rows):
        parts = []
        for h in range(H):
            lanes = slice(h * HEAD_DIM, (h + 1) * HEAD_DIM)
            parts.append(
                (
                    num_ref[h, rows, :]
                    * scale_ref[rows, 0:1]
                    * mem_gain_ref[:, lanes]
                    * silu(gate_ref[h, rows, :])
                ).astype(BF16)
            )
        return parts[0] if H == 1 else jnp.concatenate(parts, axis=1)

    links, siblings = [], []
    for j in range(1, chips + 1):
        target = lax.rem(chip + j, chips)
        for n in range(CHUNKS):
            slot = (j - 1) * CHUNKS + n
            theirs = pl.ds(
                pl.multiple_of((target * 2 + 1 - core) * block + n * size, size), size
            )
            ours = pl.ds(pl.multiple_of((target * 2 + core) * block + n * size, size), size)
            lhs_memory = jnp.concatenate([memory_out(theirs), memory_out(ours)], axis=0)
            lhs_pool = jnp.concatenate([pool_ref[theirs, :], pool_ref[ours, :]], axis=0)
            both = (dot(lhs_memory, wom[...]) + dot(lhs_pool, wop[...])).astype(BF16)
            sib_send[slot] = both[:size]
            own_ref[slot] = both[size:]
            copy = remote(
                sib_send.at[slot], sib_recv.at[slot], sib_sems, slot, "tp", sibling
            )
            copy.start()
            siblings.append(copy)
            if j < chips:
                copy.wait_recv()
                link_send[slot] = (
                    own_ref[slot].astype(F32) + sib_recv[slot].astype(F32)
                ).astype(BF16)
                hop = remote(
                    link_send.at[slot],
                    link_recv.at[slot],
                    link_sems,
                    slot,
                    "tp",
                    target * 2 + core,
                )
                hop.start()
                links.append(hop)
    for n in range(CHUNKS):
        slot = (chips - 1) * CHUNKS + n
        siblings[slot].wait_recv()
        total = own_ref[slot].astype(F32) + sib_recv[slot].astype(F32)
        for j in range(1, chips):
            other = (j - 1) * CHUNKS + n
            links[other].wait_recv()
            total = total + link_recv[other].astype(F32)
        scale = lax.rsqrt(jnp.mean(total * total, axis=-1, keepdims=True) + EPS)
        out_ref[pl.ds(n * size, size), :] = (total * scale * post_ref[...]).astype(BF16)
    for copy in siblings + links:
        copy.wait_send()


def body(
    n_sp,
    n_tp,
    tokens,
    pre_gain,
    w_query,
    w_key,
    w_value,
    memory_output_gate_weight,
    w_input_gate,
    w_forget_gate,
    input_bias,
    forget_bias,
    forget_extra,
    initial_memory,
    initial_normal,
    memory_gain,
    w_pool_input,
    w_pool_gate,
    pool_mix,
    pool_gain,
    w_out_memory,
    w_out_pool,
    post_gain,
):
    T, D = tokens.shape
    MW = w_query.shape[1]
    PW = w_pool_input.shape[1]
    H = MW // HEAD_DIM
    G = PW // GROUP_DIM
    sp, tp = lax.axis_index("sp"), lax.axis_index("tp")
    cut = functools.partial(lax.dynamic_slice_in_dim, start_index=tp * H, slice_size=H)
    gates_w = jnp.pad(
        jnp.concatenate([cut(w_input_gate, axis=1), cut(w_forget_gate, axis=1)], axis=1),
        ((0, 0), (0, 128 - 2 * H)),
    )
    gates_b = jnp.pad(
        jnp.concatenate([cut(input_bias, axis=0), cut(forget_bias, axis=0)]), (0, 128 - 2 * H)
    )[None]
    extra = jnp.pad(forget_extra.T, ((H, 8 - 2 * H), (0, 0)))
    part = initial_normal.shape[1]
    normal = lax.dynamic_update_slice(
        jnp.zeros((H, HEAD_DIM), F32), initial_normal, (0, sp * part)
    )
    mem_gain = lax.dynamic_slice_in_dim(memory_gain, tp * MW, MW, 0)[None]
    gain_pool = lax.dynamic_slice_in_dim(pool_gain, tp * PW, PW, 0)[None]
    mix = lax.dynamic_slice_in_dim(pool_mix, tp * G, G, 0)
    wire = BF16 if part % 16 == 0 else F32
    chips = n_tp // 2
    block = T // n_tp
    slots = chips * CHUNKS
    size = block // CHUNKS
    hbm = pl.BlockSpec(memory_space=pl.ANY)
    vmem = pl.BlockSpec(memory_space=pltpu.VMEM)
    V = pltpu.VMEM
    dma = pltpu.SemaphoreType.DMA
    return pl.pallas_call(
        functools.partial(kernel, n_sp, n_tp),
        out_shape=jax.ShapeDtypeStruct((block, D), BF16),
        in_specs=[hbm, vmem, hbm, hbm, hbm, hbm, vmem, vmem, vmem, vmem, vmem, vmem]
        + [hbm, hbm, vmem, vmem, hbm, hbm, vmem],
        out_specs=vmem,
        scratch_shapes=[
            V((T, D), BF16),
            V((D, MW), BF16),
            V((D, MW), BF16),
            V((D, MW), BF16),
            V((D, MW), BF16),
            V((D, PW), BF16),
            V((D, PW), BF16),
            V((MW, D), BF16),
            V((PW, D), BF16),
            V((T, D), BF16),
            V((H, T, HEAD_DIM), BF16),
            V((H, T, HEAD_DIM), BF16),
            V((H, T, HEAD_DIM), BF16),
            V((H, T, HEAD_DIM), F32),
            V((T, PW), F32),
            V((T + WIDEST, PW), BF16),
            V((T, PW), BF16),
            V((128, T), F32),
            V((T, 128), F32),
            V((H, T, HEAD_DIM), F32),
            V((H, T, 1), F32),
            V((H, T, 1), F32),
            V((n_sp, H, part, HEAD_DIM), wire),
            V((n_sp, H, part, HEAD_DIM), wire),
            V((8, HEAD_DIM), F32),
            V((n_sp, 8, HEAD_DIM), F32),
            V((n_sp, H, part, HEAD_DIM), wire),
            V((n_sp, H, part, HEAD_DIM), wire),
            V((8, T), F32),
            V((n_tp, 8, T), F32),
            V((T, 128), F32),
            V((slots, size, D), BF16),
            V((slots, size, D), BF16),
            V((slots, size, D), BF16),
            V((slots, size, D), BF16),
            V((slots, size, D), BF16),
            dma((9,)),
            dma((2, n_sp)),
            dma((2, n_sp)),
            dma((2, n_sp)),
            dma((2, 1)),
            dma((2, n_tp)),
            dma((2, slots)),
            dma((2, slots)),
        ],
        compiler_params=pltpu.CompilerParams(
            collective_id=0, has_side_effects=True, vmem_limit_bytes=60 * 1024 * 1024
        ),
    )(
        tokens,
        pre_gain[None],
        w_query,
        w_key,
        w_value,
        memory_output_gate_weight,
        gates_w,
        gates_b,
        extra,
        initial_memory,
        normal,
        mem_gain,
        w_pool_input,
        w_pool_gate,
        mix,
        gain_pool,
        w_out_memory,
        w_out_pool,
        post_gain[None],
    )


def solution(mesh):
    in_specs = (
        P("sp", None),
        P(),
        P(None, "tp"),
        P(None, "tp"),
        P(None, "tp"),
        P(None, "tp"),
        P(),
        P(),
        P(),
        P(),
        P("sp", "tp"),
        P("tp", "sp", None),
        P("tp", "sp"),
        P(),
        P(None, "tp"),
        P(None, "tp"),
        P(),
        P(),
        P("tp", None),
        P("tp", None),
        P(),
    )
    out_specs = P(("sp", "tp"), None)
    sizes = dict(mesh.shape)
    run = functools.partial(body, sizes["sp"], sizes["tp"])
    return jax.shard_map(run, mesh=mesh, in_specs=in_specs, out_specs=out_specs, check_vma=False)
```

```python
import functools

import jax
import jax.numpy as jnp
from jax import lax
from jax.experimental import pallas as pl
from jax.experimental.pallas import tpu as pltpu
from jax.sharding import PartitionSpec as P

HEAD_DIM = 256
GROUP_DIM = 128
WIDEST = 256
TILE = 256
CHUNKS = 2
EPS = 1e-06
FLOOR = -1e30
F32 = jnp.float32
BF16 = jnp.bfloat16
MESH = pl.DeviceIdType.MESH


def dot(a, b):
    return jnp.dot(a, b, preferred_element_type=F32)


def silu(x):
    return x / (1.0 + jnp.exp(-x))


def kernel(
    n_sp,
    n_tp,
    tokens_hbm,
    gain_ref,
    wq_hbm,
    wk_hbm,
    wv_hbm,
    wg_hbm,
    w_in_ref,
    w_forget_ref,
    b_in_ref,
    b_forget_ref,
    extra_ref,
    init_ref,
    normal_ref,
    mem_gain_ref,
    wpi_hbm,
    wpg_hbm,
    mix_ref,
    pool_gain_ref,
    wom_hbm,
    wop_hbm,
    post_ref,
    out_ref,
    tokens,
    wq,
    wk,
    wv,
    wg,
    wpi,
    wpg,
    wom,
    wop,
    normed,
    q_ref,
    k_ref,
    v_ref,
    gate_ref,
    pgate_ref,
    ext_ref,
    pool_ref,
    rows_ref,
    cols_ref,
    num_ref,
    den_ref,
    max_ref,
    s_send,
    s_recv,
    a_send,
    a_recv,
    e_send,
    e_recv,
    sq_send,
    sq_recv,
    scale_ref,
    sib_send,
    sib_recv,
    own_ref,
    link_send,
    link_recv,
    gates_w_ref,
    gates_b_ref,
    raw_ref,
    start_ref,
    local_sem,
    s_sems,
    a_sems,
    e_sems,
    halo_sems,
    sq_sems,
    sib_sems,
    link_sems,
):
    T, D = tokens.shape
    H = q_ref.shape[0]
    G = pool_ref.shape[1] // GROUP_DIM
    sp = lax.axis_index("sp")
    tp = lax.axis_index("tp")
    head_scale = HEAD_DIM ** (-0.5)
    tiles = T // TILE

    loads = {}
    for slot, (name, src, dst) in enumerate(
        [
            ("tokens", tokens_hbm, tokens),
            ("wk", wk_hbm, wk),
            ("wv", wv_hbm, wv),
            ("wpi", wpi_hbm, wpi),
            ("wq", wq_hbm, wq),
            ("wg", wg_hbm, wg),
            ("wpg", wpg_hbm, wpg),
            ("wop", wop_hbm, wop),
            ("wom", wom_hbm, wom),
        ]
    ):
        loads[name] = pltpu.make_async_copy(src, dst, local_sem.at[slot])
        loads[name].start()

    barrier = pltpu.get_barrier_semaphore()
    for step in range(1, n_sp):
        pl.semaphore_signal(
            barrier, inc=1, device_id={"sp": lax.rem(sp + step, n_sp)}, device_id_type=MESH
        )
    for step in range(1, n_tp):
        pl.semaphore_signal(
            barrier, inc=1, device_id={"tp": lax.rem(tp + step, n_tp)}, device_id_type=MESH
        )

    def remote(src, dst, sems, slot, axis, peer):
        return pltpu.make_async_remote_copy(
            src_ref=src,
            dst_ref=dst,
            send_sem=sems.at[0, slot],
            recv_sem=sems.at[1, slot],
            device_id={axis: peer},
            device_id_type=MESH,
        )

    def by_tile(body, size=TILE):
        def step(index, carry):
            body(pl.ds(pl.multiple_of(index * size, size), size))
            return carry

        lax.fori_loop(0, T // size, step, 0)

    heads = w_in_ref.shape[1]
    gates_w_ref[...] = jnp.zeros_like(gates_w_ref)
    gates_w_ref[:, 0:heads] = w_in_ref[...]
    gates_w_ref[:, heads : 2 * heads] = w_forget_ref[...]
    gates_b_ref[...] = jnp.zeros_like(gates_b_ref)
    gates_b_ref[:, 0:heads] = b_in_ref[...]
    gates_b_ref[:, heads : 2 * heads] = b_forget_ref[...]

    loads["tokens"].wait()

    def norm_tile(rows):
        x = tokens[rows, :].astype(F32)
        scale = lax.rsqrt(jnp.mean(x * x, axis=-1, keepdims=True) + EPS)
        normed[rows, :] = (x * scale * gain_ref[...]).astype(BF16)

    def early_products(t):
        rows = pl.ds(t * TILE, TILE)
        cols_ref[rows, :] = dot(normed[rows, :], gates_w_ref[...]) + gates_b_ref[...]
        cols_ref[rows, 2 * heads : 2 * heads + H] = extra_ref[rows, :]
        keys = dot(normed[rows, :], wk[...])
        for h in range(H):
            k_ref[h, rows, :] = keys[:, h * HEAD_DIM : (h + 1) * HEAD_DIM].astype(BF16)

    for t in range(tiles + 1):
        if t == 1:
            loads["wk"].wait()
        if t < tiles:
            for sub in range(0, TILE, 64):
                norm_tile(pl.ds(t * TILE + sub, 64))
        if t > 0:
            early_products(t - 1)
    tri = (
        lax.broadcasted_iota(jnp.int32, (TILE, TILE), 0)
        <= lax.broadcasted_iota(jnp.int32, (TILE, TILE), 1)
    ).astype(F32)
    rows_ref[...] = jnp.zeros_like(rows_ref)
    carry = jnp.zeros((8, 1), F32)
    for t in range(tiles):
        span = pl.ds(t * TILE, TILE)
        raw_ref[:, span] = cols_ref[span, :].T
        own_rows = [raw_ref[pl.ds(heads + tp * H + h, 1), span] for h in range(H)]
        added = [raw_ref[2 * heads + h : 2 * heads + h + 1, span] for h in range(H)]
        spare = [jnp.zeros((8 - H, TILE), F32)]
        raw = jnp.concatenate(own_rows + spare, axis=0)
        log_keep = jnp.minimum(raw, 0.0) - jnp.log1p(jnp.exp(-jnp.abs(raw)))
        log_keep = log_keep + jnp.concatenate(added + spare, axis=0)
        run = carry + jnp.dot(
            log_keep, tri, preferred_element_type=F32, precision=lax.Precision.HIGHEST
        )
        carry = run[:, TILE - 1 : TILE]
        for h in range(H):
            keep = run[h : h + 1]
            rows_ref[h : h + 1, span] = raw_ref[pl.ds(tp * H + h, 1), span] - keep
            rows_ref[H + h : H + h + 1, span] = keep
    for t in range(tiles):
        span = pl.ds(t * TILE, TILE)
        cols_ref[span, :] = rows_ref[:, span].T

    def project(name, weight, store):
        loads[name].wait()

        def tile(rows):
            store(rows, dot(normed[rows, :], weight[...]))

        by_tile(tile)

    def heads_to(ref):
        def store(rows, value):
            for h in range(H):
                ref[h, rows, :] = value[:, h * HEAD_DIM : (h + 1) * HEAD_DIM].astype(ref.dtype)

        return store

    project("wv", wv, heads_to(v_ref))

    part = HEAD_DIM // n_sp
    a_send[...] = jnp.zeros_like(a_send)
    for h in range(H):
        a_max = jnp.max(rows_ref[h : h + 1, :], axis=-1, keepdims=True)
        total = rows_ref[H + h : H + h + 1, T - 1 : T]
        state = jnp.zeros((HEAD_DIM, HEAD_DIM), F32)
        normal = jnp.zeros((1, HEAD_DIM), F32)
        for t in range(tiles):
            span = pl.ds(t * TILE, TILE)
            weight = jnp.exp(cols_ref[span, h : h + 1] - a_max)
            kw = weight * k_ref[h, span, :].astype(F32)
            normal = normal + jnp.sum(kw, axis=0, keepdims=True)
            state = state + lax.dot_general(
                kw.astype(BF16),
                v_ref[h, span, :],
                (((0,), (0,)), ((), ())),
                preferred_element_type=F32,
            )
        s_send[:, h] = state.reshape(n_sp, part, HEAD_DIM).astype(s_send.dtype)
        a_send[4 * h : 4 * h + 1, :] = jnp.broadcast_to(total + a_max, (1, HEAD_DIM))
        a_send[4 * h + 1 : 4 * h + 2, :] = jnp.broadcast_to(total, (1, HEAD_DIM))
        a_send[4 * h + 2 : 4 * h + 3, :] = normal
        a_send[4 * h + 3 : 4 * h + 4, 0:part] = normal_ref[h : h + 1, :]

    pl.semaphore_wait(barrier, n_sp - 1 + n_tp - 1)
    first = []
    for step in range(1, n_sp):
        peer = lax.rem(sp + step, n_sp)
        first.append(remote(s_send.at[peer], s_recv.at[sp], s_sems, step, "sp", peer))
        first.append(remote(a_send, a_recv.at[sp], a_sems, step, "sp", peer))
    for copy in first:
        copy.start()
    s_recv[sp] = s_send[sp]
    a_recv[sp] = a_send[...]

    def store_pool(rows, value):
        ext_ref[pl.ds(pl.multiple_of(rows.start + WIDEST, TILE), TILE), :] = value.astype(BF16)

    project("wpi", wpi, store_pool)
    halo = remote(
        ext_ref.at[pl.ds(T, WIDEST)],
        ext_ref.at[pl.ds(0, WIDEST)],
        halo_sems,
        0,
        "sp",
        lax.rem(sp + 1, n_sp),
    )
    halo.start()
    project("wq", wq, heads_to(q_ref))
    project("wg", wg, heads_to(gate_ref))

    for copy in first:
        copy.wait()
    enter_max, enter_normal = [], []
    for h in range(H):
        state = init_ref[h].astype(F32)
        for j in range(n_sp):
            start_ref[h : h + 1, j * part : (j + 1) * part] = a_recv[j, 4 * h + 3 : 4 * h + 4, 0:part]
        normal = start_ref[h : h + 1, :]
        stab = jnp.zeros((1, HEAD_DIM), F32)
        my_stab, my_normal = stab, normal
        for j in range(n_sp):
            e_send[j, h] = state.astype(e_send.dtype)
            my_stab = jnp.where(sp == j, stab, my_stab)
            my_normal = jnp.where(sp == j, normal, my_normal)
            late = a_recv[j, 4 * h : 4 * h + 1, :]
            keep = a_recv[j, 4 * h + 1 : 4 * h + 2, :]
            joint = jnp.maximum(late, keep + stab)
            early_factor = jnp.exp(keep + stab - joint)
            late_factor = jnp.exp(late - joint)
            state = state * early_factor + s_recv[j, h].astype(F32) * late_factor
            normal = normal * early_factor + a_recv[j, 4 * h + 2 : 4 * h + 3, :] * late_factor
            stab = joint
        enter_max.append(my_stab[:, 0:1])
        enter_normal.append(my_normal)
    second = []
    for step in range(1, n_sp):
        peer = lax.rem(sp + step, n_sp)
        second.append(remote(e_send.at[peer], e_recv.at[sp], e_sems, step, "sp", peer))
    for copy in second:
        copy.start()
    e_recv[sp] = e_send[sp]

    for h in range(H):
        for t in range(tiles):
            span = pl.ds(t * TILE, TILE)
            width = (t + 1) * TILE
            decayed = cols_ref[span, H + h : H + h + 1] + rows_ref[h : h + 1, 0:width]
            causal = (
                lax.broadcasted_iota(jnp.int32, (TILE, width), 0) + t * TILE
                >= lax.broadcasted_iota(jnp.int32, (TILE, width), 1)
            )
            decayed = jnp.where(causal, decayed, FLOOR)
            row_max = jnp.max(decayed, axis=-1, keepdims=True)
            scores = lax.dot_general(
                q_ref[h, span, :],
                k_ref[h, 0:width, :],
                (((1,), (1,)), ((), ())),
                preferred_element_type=F32,
            )
            weights = jnp.exp(decayed - row_max) * scores * head_scale
            den_ref[h, span, :] = jnp.sum(weights, axis=-1, keepdims=True)
            max_ref[h, span, :] = row_max
            num_ref[h, span, :] = dot(weights.astype(BF16), v_ref[h, 0:width, :])

    def store_gate(rows, value):
        pgate_ref[rows, :] = value

    project("wpg", wpg, store_gate)
    halo.wait()
    for g in range(G):
        window = jnp.left_shift(2, tp * G + g)
        offset = (
            lax.broadcasted_iota(jnp.int32, (TILE, TILE + WIDEST), 0)
            + WIDEST
            - lax.broadcasted_iota(jnp.int32, (TILE, TILE + WIDEST), 1)
        )
        band = jnp.where((offset >= 0) & (offset < window), 1.0, 0.0).astype(BF16)
        lanes = slice(g * GROUP_DIM, (g + 1) * GROUP_DIM)
        for t in range(tiles):
            span = pl.ds(t * TILE, TILE)
            here = ext_ref[t * TILE + WIDEST : (t + 1) * TILE + WIDEST, lanes]
            before = ext_ref[t * TILE : t * TILE + WIDEST, lanes]
            if t == 0:
                before = jnp.where(sp > 0, before.astype(F32), 0.0).astype(BF16)
            sums = dot(band[:, :WIDEST], before) + dot(band[:, WIDEST:], here)
            position = lax.broadcasted_iota(jnp.int32, (TILE, 1), 0) + (sp * T + t * TILE + 1)
            counts = jnp.minimum(position, window).astype(F32)
            pooled = (sums / counts - here.astype(F32)).astype(BF16)
            mixed = dot(pooled, mix_ref[tp * G + g])
            pool_ref[span, lanes] = (
                mixed * pool_gain_ref[:, pl.ds(pl.multiple_of((tp * G + g) * GROUP_DIM, GROUP_DIM), GROUP_DIM)] * silu(pgate_ref[span, lanes])
            ).astype(BF16)

    for copy in second:
        copy.wait()
    for t in range(tiles):
        span = pl.ds(t * TILE, TILE)
        squares = jnp.zeros((TILE, 1), F32)
        for h in range(H):
            state = e_recv[:, h].reshape(HEAD_DIM, HEAD_DIM).astype(BF16)
            queries = q_ref[h, span, :]
            carried = cols_ref[span, H + h : H + h + 1] + enter_max[h]
            row_max = max_ref[h, span, :]
            joint = jnp.maximum(row_max, carried)
            local_weight = jnp.exp(row_max - joint)
            carry_weight = jnp.exp(carried - joint) * head_scale
            numerator = num_ref[h, span, :] * local_weight + carry_weight * dot(queries, state)
            denominator = den_ref[h, span, :] * local_weight + carry_weight * jnp.sum(
                queries.astype(F32) * enter_normal[h], axis=-1, keepdims=True
            )
            memory = numerator / jnp.maximum(jnp.abs(denominator), jnp.exp(-joint))
            num_ref[h, span, :] = memory
            squares = squares + jnp.sum(memory * memory, axis=-1, keepdims=True)
        sq_send[:, span] = jnp.broadcast_to(squares, (TILE, 128)).T[0:8]

    third = []
    for step in range(1, n_tp):
        peer = lax.rem(tp + step, n_tp)
        third.append(remote(sq_send, sq_recv.at[step], sq_sems, step, "tp", peer))
    for copy in third:
        copy.start()
    loads["wop"].wait()
    loads["wom"].wait()
    for copy in third:
        copy.wait()
    for t in range(tiles):
        span = pl.ds(t * TILE, TILE)
        total = sq_send[0:1, span]
        for step in range(1, n_tp):
            total = total + sq_recv[step, 0:1, span]
        scale = lax.rsqrt(total / (HEAD_DIM * H * n_tp) + EPS)
        scale_ref[span, :] = jnp.broadcast_to(scale, (128, TILE)).T

    chips = n_tp // 2
    chip, core = tp // 2, lax.rem(tp, 2)
    sibling = chip * 2 + 1 - core
    block = T // n_tp
    size = block // CHUNKS

    def memory_out(rows):
        parts = []
        for h in range(H):
            lanes = pl.ds(pl.multiple_of((tp * H + h) * HEAD_DIM, HEAD_DIM), HEAD_DIM)
            parts.append(
                (
                    num_ref[h, rows, :]
                    * scale_ref[rows, 0:1]
                    * mem_gain_ref[:, lanes]
                    * silu(gate_ref[h, rows, :])
                ).astype(BF16)
            )
        return parts[0] if H == 1 else jnp.concatenate(parts, axis=1)

    links, siblings = [], []
    for j in range(1, chips + 1):
        target = lax.rem(chip + j, chips)
        for n in range(CHUNKS):
            slot = (j - 1) * CHUNKS + n
            theirs = pl.ds(
                pl.multiple_of((target * 2 + 1 - core) * block + n * size, size), size
            )
            ours = pl.ds(pl.multiple_of((target * 2 + core) * block + n * size, size), size)
            lhs_memory = jnp.concatenate([memory_out(theirs), memory_out(ours)], axis=0)
            lhs_pool = jnp.concatenate([pool_ref[theirs, :], pool_ref[ours, :]], axis=0)
            both = (dot(lhs_memory, wom[...]) + dot(lhs_pool, wop[...])).astype(BF16)
            sib_send[slot] = both[:size]
            own_ref[slot] = both[size:]
            copy = remote(
                sib_send.at[slot], sib_recv.at[slot], sib_sems, slot, "tp", sibling
            )
            copy.start()
            siblings.append(copy)
            if j < chips:
                copy.wait_recv()
                link_send[slot] = (
                    own_ref[slot].astype(F32) + sib_recv[slot].astype(F32)
                ).astype(BF16)
                hop = remote(
                    link_send.at[slot],
                    link_recv.at[slot],
                    link_sems,
                    slot,
                    "tp",
                    target * 2 + core,
                )
                hop.start()
                links.append(hop)
    for n in range(CHUNKS):
        slot = (chips - 1) * CHUNKS + n
        siblings[slot].wait_recv()
        total = own_ref[slot].astype(F32) + sib_recv[slot].astype(F32)
        for j in range(1, chips):
            other = (j - 1) * CHUNKS + n
            links[other].wait_recv()
            total = total + link_recv[other].astype(F32)
        scale = lax.rsqrt(jnp.mean(total * total, axis=-1, keepdims=True) + EPS)
        out_ref[pl.ds(n * size, size), :] = (total * scale * post_ref[...]).astype(BF16)
    for copy in siblings + links:
        copy.wait_send()


def body(
    n_sp,
    n_tp,
    tokens,
    pre_gain,
    w_query,
    w_key,
    w_value,
    memory_output_gate_weight,
    w_input_gate,
    w_forget_gate,
    input_bias,
    forget_bias,
    forget_extra,
    initial_memory,
    initial_normal,
    memory_gain,
    w_pool_input,
    w_pool_gate,
    pool_mix,
    pool_gain,
    w_out_memory,
    w_out_pool,
    post_gain,
):
    T, D = tokens.shape
    MW = w_query.shape[1]
    PW = w_pool_input.shape[1]
    H = MW // HEAD_DIM
    G = PW // GROUP_DIM
    part = initial_normal.shape[1]
    wire = BF16 if part % 16 == 0 else F32
    chips = n_tp // 2
    block = T // n_tp
    slots = chips * CHUNKS
    size = block // CHUNKS
    hbm = pl.BlockSpec(memory_space=pl.ANY)
    vmem = pl.BlockSpec(memory_space=pltpu.VMEM)
    V = pltpu.VMEM
    dma = pltpu.SemaphoreType.DMA
    return pl.pallas_call(
        functools.partial(kernel, n_sp, n_tp),
        out_shape=jax.ShapeDtypeStruct((block, D), BF16),
        in_specs=[hbm, vmem, hbm, hbm, hbm, hbm, vmem, vmem, vmem, vmem, vmem, vmem, vmem, vmem]
        + [hbm, hbm, vmem, vmem, hbm, hbm, vmem],
        out_specs=vmem,
        scratch_shapes=[
            V((T, D), BF16),
            V((D, MW), BF16),
            V((D, MW), BF16),
            V((D, MW), BF16),
            V((D, MW), BF16),
            V((D, PW), BF16),
            V((D, PW), BF16),
            V((MW, D), BF16),
            V((PW, D), BF16),
            V((T, D), BF16),
            V((H, T, HEAD_DIM), BF16),
            V((H, T, HEAD_DIM), BF16),
            V((H, T, HEAD_DIM), BF16),
            V((H, T, HEAD_DIM), F32),
            V((T, PW), F32),
            V((T + WIDEST, PW), BF16),
            V((T, PW), BF16),
            V((128, T), F32),
            V((T, 128), F32),
            V((H, T, HEAD_DIM), F32),
            V((H, T, 1), F32),
            V((H, T, 1), F32),
            V((n_sp, H, part, HEAD_DIM), wire),
            V((n_sp, H, part, HEAD_DIM), wire),
            V((8, HEAD_DIM), F32),
            V((n_sp, 8, HEAD_DIM), F32),
            V((n_sp, H, part, HEAD_DIM), wire),
            V((n_sp, H, part, HEAD_DIM), wire),
            V((8, T), F32),
            V((n_tp, 8, T), F32),
            V((T, 128), F32),
            V((slots, size, D), BF16),
            V((slots, size, D), BF16),
            V((slots, size, D), BF16),
            V((slots, size, D), BF16),
            V((slots, size, D), BF16),
            V((D, 128), BF16),
            V((1, 128), F32),
            V((128, T), F32),
            V((8, HEAD_DIM), F32),
            dma((9,)),
            dma((2, n_sp)),
            dma((2, n_sp)),
            dma((2, n_sp)),
            dma((2, 1)),
            dma((2, n_tp)),
            dma((2, slots)),
            dma((2, slots)),
        ],
        compiler_params=pltpu.CompilerParams(
            collective_id=0, has_side_effects=True, vmem_limit_bytes=60 * 1024 * 1024
        ),
    )(
        tokens,
        pre_gain[None],
        w_query,
        w_key,
        w_value,
        memory_output_gate_weight,
        w_input_gate,
        w_forget_gate,
        input_bias[None],
        forget_bias[None],
        forget_extra,
        initial_memory,
        initial_normal,
        memory_gain[None],
        w_pool_input,
        w_pool_gate,
        pool_mix,
        pool_gain[None],
        w_out_memory,
        w_out_pool,
        post_gain[None],
    )


def solution(mesh):
    in_specs = (
        P("sp", None),
        P(),
        P(None, "tp"),
        P(None, "tp"),
        P(None, "tp"),
        P(None, "tp"),
        P(),
        P(),
        P(),
        P(),
        P("sp", "tp"),
        P("tp", "sp", None),
        P("tp", "sp"),
        P(),
        P(None, "tp"),
        P(None, "tp"),
        P(),
        P(),
        P("tp", None),
        P("tp", None),
        P(),
    )
    out_specs = P(("sp", "tp"), None)
    sizes = dict(mesh.shape)
    run = functools.partial(body, sizes["sp"], sizes["tp"])
    return jax.shard_map(run, mesh=mesh, in_specs=in_specs, out_specs=out_specs, check_vma=False)
```
